32 devices in a mesh: ep: 8 (over z, x), tp: 4 (over y, core).
Axes of the slice: x: 2, y: 2, z: 4, core: 2. Of those that a mesh axis runs over, the one named last changes fastest.
Arguments:
- tokens_first: bfloat16 [4096, 2048], P('ep'), may hold values from -6 to 6
- attn_gain: float32 [2048], replicated, may hold values from 0.1 to 1.9
- w_query: bfloat16 [2048, 1024], P(None, 'tp'), may hold values from -6 to 6
- key_matrix: bfloat16 [2048, 512], P(None, 'tp'), may hold values from -6 to 6
- value_matrix: bfloat16 [2048, 512], P(None, 'tp'), may hold values from -0.125 to 0.125
- head_sink_logit: float32 [16], P('tp'), may hold values from 1 to 5
- w_output: bfloat16 [1024, 2048], P('tp'), may hold values from -0.75 to 0.75
- tokens_second: bfloat16 [1024, 2048], P('ep'), may hold values from -6 to 6
- ffn_gain: float32 [2048], replicated, may hold values from 0.1 to 1.9
- routes: int32 [1024, 4], P('ep'), may hold values from 0 to 15, all different within a row; in each aligned block of 128 rows (0 to 127, 128 to 255, ...) at most 64 rows name the same one
- route_weight: float32 [1024, 4], P('ep'), may hold values from 0.2 to 1.5
- w_gate_exp: bfloat16 [16, 2048, 2048], P('ep', None, 'tp'), may hold values from -0.125 to 0.125
- w_up_exp: bfloat16 [16, 2048, 2048], P('ep', None, 'tp'), may hold values from -0.125 to 0.125
- w_down_exp: bfloat16 [16, 2048, 2048], P('ep', 'tp'), may hold values from -0.125 to 0.125
- w_gate_shared: bfloat16 [2048, 1024], P(None, 'tp'), may hold values from -0.125 to 0.125
- w_up_shared: bfloat16 [2048, 1024], P(None, 'tp'), may hold values from -0.125 to 0.125
- w_down_shared: bfloat16 [1024, 2048], P('tp'), may hold values from -0.1875 to 0.1875
Outputs:
- mixer_out: bfloat16 [4096, 2048], P(('ep', 'tp'))
- moe_out: bfloat16 [1024, 2048], P('ep', 'tp')
The draws below stay inside these ranges and needn't reach their ends.
Inputs may be any that keep to these rules, and one draw needn't show every extreme that they name: `routes`: each row names 4 different experts; among the rows of one index of ep no expert is named more than 64 times, a bound that some block reaches.
All inputs are finite; a program needn't handle non-finite values.
Results may differ from the reference program's by a relative error of at most 0.017.
Values may be sent and summed in bfloat16 or wider, within the bound.
A program may use at most 64 MiB of HBM per device.

```python
import math
import jax
import jax.numpy as jnp
import numpy as np
from jax import lax

MODEL_WIDTH = 2048
HEAD_SIZE = 64
QUERY_HEADS = 16
KEY_VALUE_HEADS = 8
BAND_LENGTH = 128
EFF = 2048
SFF = 1024
TOPK = 4
TOK1_DEV = 512
TOK2_DEV = 128
EXPERTS = 16
CAP = 64
TOKENS1 = 4096
TOKENS2 = 1024
N_EP = 8
N_TP = 4


def key_lookup(key):
    rotary_base = jax.random.normal(jax.random.fold_in(key, 7), (MODEL_WIDTH, KEY_VALUE_HEADS * HEAD_SIZE), jnp.float32)
    return jnp.clip(rotary_base, -6.0, 6.0) / math.sqrt(MODEL_WIDTH)


def draw_key_matrix(key, part):
    return key_lookup(key).astype(jnp.bfloat16)


def draw_w_query(key, part):
    rotary_base = jnp.clip(jax.random.normal(jax.random.fold_in(key, 11), (MODEL_WIDTH, QUERY_HEADS * HEAD_SIZE), jnp.float32), -6.0, 6.0) / math.sqrt(MODEL_WIDTH)
    return jnp.clip(rotary_base, -6.0, 6.0).astype(jnp.bfloat16)


def shard_levels(stream_key, dims, pieces, smallest, high):
    loudness = 1.0
    for position, shards_of in pieces:
        heights = jax.random.uniform(jax.random.fold_in(jax.random.fold_in(stream_key, 6), position), (shards_of,), jnp.float32, smallest / len(pieces), high / len(pieces))
        loudness = loudness * jnp.repeat(jnp.exp(heights), dims[position] // shards_of).reshape((-1,) + (1,) * (len(dims) - 1 - position))
    return loudness


def assign_block(key, own, number, rows, number_of, top, most, lean):
    ranking = jax.random.permutation(key, number_of)
    crowded, ordinary = portions_of(number_of, rows * top, most, lean, True), portions_of(number_of, rows * top, most, lean, False)
    places = jnp.arange(number_of)

    def named(tallies, offset_by):
        used = int((tallies > 0).sum())
        fixed = max(1, used // 4)
        shifted = fixed + (places - fixed + offset_by * (used - fixed)) % max(1, number_of - fixed)
        return jnp.zeros((number_of,), jnp.int32).at[ranking[jnp.where(places < fixed, places, shifted)]].set(jnp.asarray(tallies, jnp.int32))

    tallies = jnp.where(number % 4 == 0, named(crowded, number // 4), named(ordinary, number - number // 4 - 1))
    mixed = jax.random.permutation(jax.random.fold_in(own, 3), number_of)
    source_of, receiver = mixed[0:number_of // 2 * 2:2], mixed[1:number_of // 2 * 2:2]
    margin = jnp.minimum(tallies[source_of] - 1, most - tallies[receiver]) // 2
    margin = jnp.where((source_of == ranking[0]) | (receiver == ranking[0]) | (tallies[receiver] == 0), 0, jnp.maximum(margin, 0))
    shifted = jax.random.randint(jax.random.fold_in(own, 4), (number_of // 2,), 0, 1 << 20) % (margin + 1)
    tallies = tallies.at[source_of].add(-shifted).at[receiver].add(shifted)
    labels = jnp.searchsorted(jnp.cumsum(tallies), jnp.arange(rows * top), side="right").astype(jnp.int32)
    listing = labels.reshape(top, rows).T
    listing = listing[jax.random.permutation(jax.random.fold_in(own, 1), rows)]
    offset_by = jax.random.randint(jax.random.fold_in(own, 2), (rows, 1), 0, top)
    return jnp.take_along_axis(listing, (jnp.arange(top)[None, :] + offset_by) % top, axis=1)


def portions_of(number_of, total, bound, lean, full):
    portions = [(1 << 20) // math.isqrt(rank ** lean) + 1 for rank in range(1, number_of + 1)]
    largest = bound if full else min(bound, max(-(-total // number_of), total * portions[0] // sum(portions)))
    least = 1 if total - largest >= number_of - 1 else 0
    given, surplus = [largest] + [least] * (number_of - 1), total - largest - least * (number_of - 1)
    while surplus > 0:
        free = [i for i in range(1, number_of) if given[i] < largest] or [i for i in range(1, number_of) if given[i] < bound]
        mass, left = sum([portions[i] for i in free]), surplus
        for i in free:
            extra = min(bound - given[i], max(1, left * portions[i] // mass), surplus)
            given[i] = given[i] + extra
            surplus = surplus - extra
    return np.array(given)


def scatter_about(key, extent, spread, bound, pieces=(), kind=jnp.bfloat16):
    level = shard_levels(key, extent, pieces, -0.22, 0.18) if pieces else 1.0
    values = jax.random.normal(key, extent, jnp.float32) * spread * level
    return jnp.minimum(jnp.maximum(values, -bound), bound).astype(kind)


def setup_inputs(seed: int = 0) -> dict:
    arg_keys = jax.random.split(jax.random.key(seed), 18)
    tokens_first = scatter_about(arg_keys[0], (TOKENS1, MODEL_WIDTH), 1.0, 6.0, ((0, 8),))
    attn_gain = jnp.clip(1.0 + 0.18 * jax.random.normal(arg_keys[1], (MODEL_WIDTH,), jnp.float32), 0.1, 1.9)
    w_query = draw_w_query(jax.random.fold_in(arg_keys[17], 71), 0)
    key_matrix = draw_key_matrix(jax.random.fold_in(arg_keys[17], 71), 0)
    value_matrix = scatter_about(arg_keys[4], (MODEL_WIDTH, KEY_VALUE_HEADS * HEAD_SIZE), MODEL_WIDTH ** -0.5, 0.125, ((1, 4),))
    head_sink_logit = jnp.clip(1.0 + 4.0 * jax.random.uniform(arg_keys[5], (QUERY_HEADS,), jnp.float32) ** shard_levels(arg_keys[5], (QUERY_HEADS,), ((0, 4),), -0.2, 0.2), 1.0, 5.0)
    w_output = scatter_about(arg_keys[6], (QUERY_HEADS * HEAD_SIZE, MODEL_WIDTH), (QUERY_HEADS * HEAD_SIZE // 16) ** -0.5, 0.75, ((0, 4),))
    tokens_second = scatter_about(arg_keys[7], (TOKENS2, MODEL_WIDTH), 1.0, 6.0, ((0, 8),))
    ffn_gain = jnp.clip(1.0 + 0.18 * jax.random.normal(arg_keys[8], (MODEL_WIDTH,), jnp.float32), 0.1, 1.9)
    routes_keys = jax.random.split(jax.random.fold_in(arg_keys[9], 1), TOKENS2 // TOK2_DEV)
    routes_turns = jax.random.permutation(jax.random.fold_in(arg_keys[9], 3), TOKENS2 // TOK2_DEV)
    routes = jax.vmap(lambda own, number: assign_block(jax.random.fold_in(arg_keys[9], 2), own, number, TOK2_DEV, EXPERTS, TOPK, CAP, 2))(routes_keys, routes_turns).reshape((TOKENS2, TOPK))
    route_weight = jnp.clip(0.2 + 1.3 * jax.random.uniform(arg_keys[10], (TOKENS2, TOPK), jnp.float32) ** shard_levels(arg_keys[10], (TOKENS2, TOPK), ((0, 8),), -0.2, 0.2), 0.2, 1.5)
    w_gate_exp = scatter_about(arg_keys[11], (EXPERTS, MODEL_WIDTH, EFF), MODEL_WIDTH ** -0.5, 0.125, ((0, 8), (2, 4)))
    w_up_exp = scatter_about(arg_keys[12], (EXPERTS, MODEL_WIDTH, EFF), MODEL_WIDTH ** -0.5, 0.125, ((0, 8), (2, 4)))
    w_down_exp = scatter_about(arg_keys[13], (EXPERTS, EFF, MODEL_WIDTH), EFF ** -0.5, 0.125, ((0, 8), (1, 4)))
    w_gate_shared = scatter_about(arg_keys[14], (MODEL_WIDTH, SFF), MODEL_WIDTH ** -0.5, 0.125, ((1, 4),))
    w_up_shared = scatter_about(arg_keys[15], (MODEL_WIDTH, SFF), MODEL_WIDTH ** -0.5, 0.125, ((1, 4),))
    w_down_shared = scatter_about(arg_keys[16], (SFF, MODEL_WIDTH), SFF ** -0.5, 0.1875, ((0, 4),))
    return dict(tokens_first=tokens_first, attn_gain=attn_gain, w_query=w_query, key_matrix=key_matrix, value_matrix=value_matrix, head_sink_logit=head_sink_logit, w_output=w_output, tokens_second=tokens_second, ffn_gain=ffn_gain, routes=routes, route_weight=route_weight, w_gate_exp=w_gate_exp, w_up_exp=w_up_exp, w_down_exp=w_down_exp, w_gate_shared=w_gate_shared, w_up_shared=w_up_shared, w_down_shared=w_down_shared)


rope_base = 10000.0
norm_eps = 1e-06

def rms_scale(inputs, gain):
    wide = inputs.astype(jnp.float32)
    scaled = wide * lax.rsqrt(lax.optimization_barrier(jnp.mean(wide * wide, axis=-1, keepdims=True)) + norm_eps)
    return (scaled * gain).astype(jnp.bfloat16)

def apply_rotary(heads, token_positions):
    freqs = rope_base ** (-jnp.arange(0, HEAD_SIZE, 2, dtype=jnp.float32) / HEAD_SIZE)
    angles = token_positions[:, None] * freqs[None, :]
    cosine = jnp.cos(angles)[:, None, :]
    sine = jnp.sin(angles)[:, None, :]
    first_half, second_half = jnp.split(heads, 2, axis=-1)
    return jnp.concatenate([first_half * cosine - second_half * sine, second_half * cosine + first_half * sine], axis=-1)

def group_sum(rows, weights, groups):
    width = rows.shape[1] // groups
    parts = jnp.einsum('rtc,tcd->trd', rows.reshape(rows.shape[0], groups, width).astype(jnp.float32), weights.reshape(groups, width, weights.shape[1]).astype(jnp.float32))
    return lax.optimization_barrier(jnp.sum(parts.astype(jnp.bfloat16).astype(jnp.float32), axis=0))

def reference(tokens_first, attn_gain, w_query, key_matrix, value_matrix, head_sink_logit, w_output, tokens_second, ffn_gain, routes, route_weight, w_gate_exp, w_up_exp, w_down_exp, w_gate_shared, w_up_shared, w_down_shared):
    first_count = tokens_first.shape[0]
    norm_input = rms_scale(tokens_first, attn_gain)
    token_positions = jnp.arange(first_count, dtype=jnp.int32).astype(jnp.float32)
    query_rows = apply_rotary(jnp.dot(norm_input, w_query, preferred_element_type=jnp.float32).reshape(first_count, QUERY_HEADS, HEAD_SIZE), token_positions).astype(jnp.bfloat16)
    key_rows = apply_rotary(jnp.dot(norm_input, key_matrix, preferred_element_type=jnp.float32).reshape(first_count, KEY_VALUE_HEADS, HEAD_SIZE), token_positions).astype(jnp.bfloat16)
    value_rows = jnp.dot(norm_input, value_matrix, preferred_element_type=jnp.float32).astype(jnp.bfloat16).reshape(first_count, KEY_VALUE_HEADS, HEAD_SIZE)
    pad_rows = jnp.zeros((BAND_LENGTH, KEY_VALUE_HEADS, HEAD_SIZE), jnp.bfloat16)
    keys_padded = jnp.concatenate([pad_rows, key_rows], axis=0)
    values_padded = jnp.concatenate([pad_rows, value_rows], axis=0)
    layer_block = min(512, TOK1_DEV)
    head_group = QUERY_HEADS // KEY_VALUE_HEADS
    sink_scores = head_sink_logit.astype(jnp.float32).reshape(KEY_VALUE_HEADS, head_group)[:, :, None, None]

    def attend(index):
        leading_row = index * layer_block
        block_queries = lax.dynamic_slice_in_dim(query_rows, leading_row, layer_block, 0).reshape(layer_block, KEY_VALUE_HEADS, head_group, HEAD_SIZE).astype(jnp.float32)
        key_block = lax.dynamic_slice_in_dim(keys_padded, leading_row, layer_block + BAND_LENGTH, 0).astype(jnp.float32)
        value_block = lax.dynamic_slice_in_dim(values_padded, leading_row, layer_block + BAND_LENGTH, 0).astype(jnp.float32)
        scores = jnp.einsum('qhgd,khd->hgqk', block_queries, key_block) * HEAD_SIZE ** (-0.5)
        query_pos = leading_row + jnp.arange(layer_block, dtype=jnp.int32)
        key_pos = leading_row - BAND_LENGTH + jnp.arange(layer_block + BAND_LENGTH, dtype=jnp.int32)
        offsets = query_pos[:, None] - key_pos[None, :]
        visible = (offsets >= 0) & (offsets < BAND_LENGTH) & (key_pos[None, :] >= 0)
        scores = jnp.where(visible[None, None], scores, -jnp.inf)
        peak = jnp.maximum(lax.optimization_barrier(jnp.max(scores, axis=-1, keepdims=True)), sink_scores)
        expo = jnp.exp(scores - peak)
        total = lax.optimization_barrier(jnp.sum(expo, axis=-1, keepdims=True)) + jnp.exp(sink_scores - peak)
        weights = (expo / total).astype(jnp.bfloat16)
        mixed = jnp.einsum('hgqk,khd->qhgd', weights.astype(jnp.float32), value_block)
        return mixed.astype(jnp.bfloat16).reshape(layer_block, QUERY_HEADS * HEAD_SIZE)
    attended = lax.map(attend, jnp.arange(first_count // layer_block, dtype=jnp.int32)).reshape(first_count, QUERY_HEADS * HEAD_SIZE)

    def project(rows):
        return group_sum(rows, w_output, N_TP).astype(jnp.bfloat16)
    mixer_out = lax.map(project, attended.reshape(N_EP, TOK1_DEV, QUERY_HEADS * HEAD_SIZE)).reshape(first_count, MODEL_WIDTH)
    count_second = tokens_second.shape[0]
    normed_second = rms_scale(tokens_second, ffn_gain)
    flat = routes.reshape(N_EP, TOK2_DEV * TOPK)
    onehot = (flat[:, :, None] == jnp.arange(EXPERTS, dtype=jnp.int32)[None, None, :]).astype(jnp.int32)
    ranks = lax.optimization_barrier(jnp.sum((jnp.cumsum(onehot, axis=1) - onehot) * onehot, axis=-1))
    sources = jnp.arange(N_EP, dtype=jnp.int32)[:, None]
    slots = (flat * (N_EP * CAP) + sources * CAP + ranks).reshape(count_second * TOPK).astype(jnp.int32)
    row_ids = jnp.repeat(jnp.arange(count_second, dtype=jnp.int32), TOPK)
    buffer = jnp.zeros((EXPERTS * N_EP * CAP, MODEL_WIDTH), jnp.bfloat16).at[slots].set(normed_second[row_ids])

    def expert(operands):
        rows, gate_w, up_w, down_w = operands
        gate_pre = jnp.dot(rows, gate_w, preferred_element_type=jnp.float32)
        up_pre = jnp.dot(rows, up_w, preferred_element_type=jnp.float32)
        hidden = (jax.nn.silu(gate_pre) * up_pre).astype(jnp.bfloat16)
        return group_sum(hidden, down_w, N_TP).astype(jnp.bfloat16)
    results = lax.map(expert, (buffer.reshape(EXPERTS, N_EP * CAP, MODEL_WIDTH), w_gate_exp, w_up_exp, w_down_exp)).reshape(-1, MODEL_WIDTH)
    chosen = results[slots].reshape(count_second, TOPK, MODEL_WIDTH).astype(jnp.float32)
    routed = lax.optimization_barrier(jnp.sum(chosen * route_weight.astype(jnp.float32)[:, :, None], axis=1))
    shared_hidden = (jax.nn.silu(jnp.dot(normed_second, w_gate_shared, preferred_element_type=jnp.float32)) * jnp.dot(normed_second, w_up_shared, preferred_element_type=jnp.float32)).astype(jnp.bfloat16)
    shared_sum = group_sum(shared_hidden, w_down_shared, N_TP)
    moe_out = (routed + shared_sum).astype(jnp.bfloat16)
    return (mixer_out, moe_out)
```

```python
import functools
import jax
import jax.numpy as jnp
from jax import lax
from jax.experimental import pallas as pl
from jax.experimental.pallas import tpu as pltpu
from jax.sharding import PartitionSpec as P

MODEL_WIDTH = 2048
HEAD_SIZE = 64
BAND_LENGTH = 128


rope_base = 10000.0
norm_eps = 1e-06


def from_behind(value, axis, by):
    devices = lax.axis_size(axis)
    pairs = [(i, i + by) for i in range(devices) if 0 <= i + by < devices]
    return lax.ppermute(value, axis, pairs)


def rms_scale(inputs, gain):
    wide = inputs.astype(jnp.float32)
    scaled = wide * lax.rsqrt(jnp.mean(wide * wide, axis=-1, keepdims=True) + norm_eps)
    return (scaled * gain).astype(jnp.bfloat16)


def apply_rotary(heads, token_positions):
    freqs = rope_base ** (-jnp.arange(0, HEAD_SIZE, 2, dtype=jnp.float32) / HEAD_SIZE)
    angles = token_positions[:, None] * freqs[None, :]
    cosine = jnp.cos(angles)[:, None, :]
    sine = jnp.sin(angles)[:, None, :]
    first_half, second_half = jnp.split(heads, 2, axis=-1)
    return jnp.concatenate(
        [first_half * cosine - second_half * sine, second_half * cosine + first_half * sine],
        axis=-1,
    )


MESH = pl.DeviceIdType.MESH


def whereabouts():
    me, t = lax.axis_index("ep"), lax.axis_index("tp")
    z, x, y, c = me // 2, me % 2, t // 2, t % 2
    zs = (z, z + 1 - 2 * (z % 2), (z + 2) % 4, 3 - z)
    return me, x, y, c, zs


def cols(yy, cc, width):
    return pl.ds(pl.multiple_of((yy * 2 + cc) * width, 128), width)


def rows_of(index, count):
    return pl.ds(pl.multiple_of(index * count, 16), count)


def gather_kernel(
    n_ep, x_ref, meta_ref, halo_ref, out_ref, meta_out, halo_out,
    zs_, zr_, xs_, xr_, ys_, yr_, cs_, cr_, ms_, mr_, hs_, hr_,
):
    me, x, y, c, zs = whereabouts()
    rows, width = x_ref.shape[0], x_ref.shape[1] // 4
    z_peer = [{"ep": zd * 2 + x, "tp": y * 2 + c} for zd in zs]
    x_peer = {"ep": zs[0] * 2 + 1 - x, "tp": y * 2 + c}
    y_peer = {"ep": me, "tp": (1 - y) * 2 + c}
    c_peer = {"ep": me, "tp": y * 2 + 1 - c}
    barrier = pltpu.get_barrier_semaphore()
    for e in range(1, n_ep):
        pl.semaphore_signal(
            barrier, inc=1, device_id={"ep": (me + e) % n_ep, "tp": y * 2 + c}, device_id_type=MESH
        )
    for peer in (y_peer, c_peer):
        pl.semaphore_signal(barrier, inc=1, device_id=peer, device_id_type=MESH)
    pl.semaphore_wait(barrier, n_ep + 1)

    started = []

    def make(blk, yy, peer, send, recv, own=False):
        at = out_ref.at[rows_of(blk, rows), cols(yy, c, width)]
        return pltpu.make_async_remote_copy(
            src_ref=x_ref.at[:, cols(yy, c, width)] if own else at,
            dst_ref=at, send_sem=send, recv_sem=recv, device_id=peer, device_id_type=MESH,
        )

    def go(*a, **k):
        copy = make(*a, **k)
        copy.start()
        started.append(copy)

    for d in (3, 2, 1):
        go(me, y, z_peer[d], zs_.at[d], zr_.at[d], own=True)
    go(me, y, x_peer, xs_.at[0], xr_.at[0], own=True)
    go(me, 1 - y, z_peer[1], zs_.at[0], zr_.at[0], own=True)
    go(me, 1 - y, x_peer, xs_.at[4], xr_.at[4], own=True)

    def meta_copy(e, to):
        return pltpu.make_async_remote_copy(
            src_ref=meta_ref, dst_ref=meta_out.at[to], send_sem=ms_.at[e], recv_sem=mr_.at[e],
            device_id={"ep": (me + e) % n_ep, "tp": y * 2 + c}, device_id_type=MESH,
        )

    for e in range(1, n_ep):
        meta_copy(e, me).start()
    halo = pltpu.make_async_remote_copy(
        src_ref=halo_ref, dst_ref=halo_out, send_sem=hs_, recv_sem=hr_,
        device_id={"ep": (me + 1) % n_ep, "tp": y * 2 + c}, device_id_type=MESH,
    )

    @pl.when(me < n_ep - 1)
    def _():
        halo.start()

    @pl.when(me == 0)
    def _():
        halo_out[...] = jnp.zeros_like(halo_out)

    out_ref[rows_of(me, rows), :] = x_ref[...]
    meta_out[me] = meta_ref[...]

    c_list = []

    def arrived(blk, yy, sem, peer):
        make(blk, yy, peer, sem, sem).wait_recv()

    def to_core(blk, yy):
        i = len(c_list)
        c_list.append((blk, yy))
        go(blk, yy, c_peer, cs_.at[i], cr_.at[i])

    y_list = []

    def to_y(blk):
        i = len(y_list)
        y_list.append(blk)
        go(blk, y, y_peer, ys_.at[i], yr_.at[i])

    def blk(d, xx):
        return zs[d] * 2 + xx

    for d in (1, 2, 3):
        arrived(blk(d, x), y, zr_.at[d], c_peer)
        go(blk(d, x), y, x_peer, xs_.at[d], xr_.at[d])
        if d != 1:
            to_y(blk(d, x))
        to_core(blk(d, x), y)
    arrived(blk(0, 1 - x), y, xr_.at[0], c_peer)
    to_core(blk(0, 1 - x), y)
    arrived(blk(1, x), 1 - y, zr_.at[0], c_peer)
    to_core(blk(1, x), 1 - y)
    arrived(blk(0, 1 - x), 1 - y, xr_.at[4], c_peer)
    to_core(blk(0, 1 - x), 1 - y)
    for d in (1, 2, 3):
        arrived(blk(d, 1 - x), y, xr_.at[d], c_peer)
        to_y(blk(d, 1 - x))
        to_core(blk(d, 1 - x), y)
    for i, b in enumerate(list(y_list)):
        arrived(b, 1 - y, yr_.at[i], c_peer)
        to_core(b, 1 - y)
    for i, (b, yy) in enumerate(c_list):
        at = out_ref.at[rows_of(b, rows), cols(yy, 1 - c, width)]
        pltpu.make_async_remote_copy(
            src_ref=at, dst_ref=at, send_sem=cs_.at[i], recv_sem=cr_.at[i],
            device_id=c_peer, device_id_type=MESH,
        ).wait_recv()
    for e in range(1, n_ep):
        meta_copy(e, (me + n_ep - e) % n_ep).wait_recv()

    @pl.when(me > 0)
    def _():
        halo.wait_recv()

    @pl.when(me < n_ep - 1)
    def _():
        halo.wait_send()

    for copy in started:
        copy.wait_send()
    for e in range(1, n_ep):
        meta_copy(e, me).wait_send()


def gather(x, meta, halo, n_ep):
    rows, wide = x.shape
    dma = pltpu.SemaphoreType.DMA
    vm = pl.BlockSpec(memory_space=pltpu.VMEM)
    return pl.pallas_call(
        functools.partial(gather_kernel, n_ep),
        out_shape=(
            jax.ShapeDtypeStruct((n_ep * rows, wide), x.dtype),
            jax.ShapeDtypeStruct((n_ep,) + meta.shape, meta.dtype),
            jax.ShapeDtypeStruct(halo.shape, halo.dtype),
        ),
        in_specs=[vm] * 3,
        out_specs=(vm, vm, vm),
        scratch_shapes=[
            dma((4,)), dma((4,)), dma((5,)), dma((5,)), dma((5,)), dma((5,)),
            dma((14,)), dma((14,)), dma((n_ep,)), dma((n_ep,)), dma, dma,
        ],
        compiler_params=pltpu.CompilerParams(
            collective_id=0, has_side_effects=True, vmem_limit_bytes=40 * 1024 * 1024
        ),
        name="gather_rows",
    )(x, meta, halo)


def ffn_kernel(
    cap, x_ref, meta_ref, wg_ref, wu_ref, wd_ref, sg_ref, su_ref, sd_ref, out_ref, xs, ys
):
    w_count = ys.shape[1] // cap
    j = pl.program_id(0)
    exp_dev = pl.num_programs(0)
    me = lax.axis_index("ep")
    n_ep, _, rows = meta_ref.shape
    topk = meta_ref.shape[1] // 2
    f32 = jnp.float32
    before = (
        lax.broadcasted_iota(jnp.int32, (rows, rows), 0)
        < lax.broadcasted_iota(jnp.int32, (rows, rows), 1)
    ).astype(f32).astype(jnp.bfloat16)

    def placed(s, jj, weighted):
        e = (me * exp_dev + jj).astype(f32)
        named = meta_ref[s, 0:topk, :] == e
        hit = jnp.sum(named.astype(f32), axis=0, keepdims=True)
        rank = jnp.dot(
            jnp.broadcast_to(hit, (16, rows)).astype(jnp.bfloat16), before,
            preferred_element_type=f32,
        )[0:1]
        slot = lax.broadcasted_iota(jnp.int32, (cap, rows), 0).astype(f32)
        value = hit
        if weighted:
            value = jnp.sum(
                jnp.where(named, meta_ref[s, topk : 2 * topk, :], 0.0), axis=0, keepdims=True
            )
        return jnp.where((slot == rank) & (hit > 0.0), value, 0.0)

    for s in range(n_ep):
        xs[pl.ds(s * cap, cap), :] = jnp.dot(
            placed(s, j, False).astype(jnp.bfloat16), x_ref[pl.ds(s * rows, rows), :],
            preferred_element_type=f32,
        ).astype(jnp.bfloat16)
    rows_in = xs[...]
    gate = jnp.dot(rows_in, wg_ref[0], preferred_element_type=f32)
    up = jnp.dot(rows_in, wu_ref[0], preferred_element_type=f32)
    hidden = (gate / (1.0 + jnp.exp(-gate)) * up).astype(jnp.bfloat16)
    res = jnp.dot(hidden, wd_ref[0], preferred_element_type=f32).astype(jnp.bfloat16)
    for s in range(n_ep):
        ys[s, pl.ds(pl.multiple_of(j * cap, cap), cap), :] = res[s * cap : (s + 1) * cap]

    @pl.when(j == exp_dev - 1)
    def _():
        for s in range(n_ep):
            mix = jnp.concatenate([placed(s, jj, True) for jj in range(w_count)], axis=0)
            out_ref[pl.ds(s * rows, rows), :] = jnp.dot(
                mix.T.astype(jnp.bfloat16), ys[s], preferred_element_type=f32
            ).astype(jnp.bfloat16)
        mine = rows_of(me, rows)
        own = x_ref[mine, :]
        sg = jnp.dot(own, sg_ref[...], preferred_element_type=f32)
        su = jnp.dot(own, su_ref[...], preferred_element_type=f32)
        sh = (sg / (1.0 + jnp.exp(-sg)) * su).astype(jnp.bfloat16)
        out_ref[mine, :] = (
            out_ref[mine, :].astype(f32) + jnp.dot(sh, sd_ref[...], preferred_element_type=f32)
        ).astype(jnp.bfloat16)


def experts_of(x, meta, wg, wu, wd, sg, su, sd, cap):
    n_ep, _, rows = meta.shape
    exp_dev, wide, hid = wg.shape
    vm = pl.BlockSpec(memory_space=pltpu.VMEM)
    return pl.pallas_call(
        functools.partial(ffn_kernel, cap),
        grid=(exp_dev,),
        out_shape=jax.ShapeDtypeStruct(x.shape, jnp.bfloat16),
        in_specs=[
            vm, vm,
            pl.BlockSpec((1, wide, hid), lambda j: (j, 0, 0)),
            pl.BlockSpec((1, wide, hid), lambda j: (j, 0, 0)),
            pl.BlockSpec((1, hid, wide), lambda j: (j, 0, 0)),
            vm, vm, vm,
        ],
        out_specs=vm,
        scratch_shapes=[
            pltpu.VMEM((n_ep * cap, wide), jnp.bfloat16),
            pltpu.VMEM((n_ep, exp_dev * cap, wide), jnp.bfloat16),
        ],
        compiler_params=pltpu.CompilerParams(
            dimension_semantics=("arbitrary",), vmem_limit_bytes=58 * 1024 * 1024
        ),
        name="experts",
    )(x, meta, wg, wu, wd, sg, su, sd)


def reduce_kernel(
    moe_ref, mix_ref, moe_out, mix_out, rc, s1, rx, s2, keep, ry, s3, rz, mrc, ms, mry,
    cs_, cr_, xs_, xr_, ys_, yr_, zs_, zr_, ms_, mr_,
):
    me, x, y, c, zs = whereabouts()
    rows, width = moe_out.shape
    mrows = mix_out.shape[0]
    f32 = jnp.float32
    x_peer = {"ep": zs[0] * 2 + 1 - x, "tp": y * 2 + c}
    y_peer = {"ep": me, "tp": (1 - y) * 2 + c}
    c_peer = {"ep": me, "tp": y * 2 + 1 - c}
    z_peer = [{"ep": zd * 2 + x, "tp": y * 2 + c} for zd in zs]
    barrier = pltpu.get_barrier_semaphore()
    for peer in [x_peer, y_peer, c_peer] + z_peer[1:]:
        pl.semaphore_signal(barrier, inc=1, device_id=peer, device_id_type=MESH)
    pl.semaphore_wait(barrier, 6)
    started = []

    def copy(src, dst, peer, send, recv):
        return pltpu.make_async_remote_copy(
            src_ref=src, dst_ref=dst, send_sem=send, recv_sem=recv,
            device_id=peer, device_id_type=MESH,
        )

    def go(*a):
        k = copy(*a)
        k.start()
        started.append(k)

    def got(dst, recv):
        copy(dst, dst, c_peer, recv, recv).wait_recv()

    ysel = (1 - y, y)
    order = (2, 3, 1, 0)

    def mine(d, xx, yy, cc):
        return (rows_of(zs[d] * 2 + xx, rows), cols(yy, cc, width))

    def mixer_core(k):
        go(
            mix_ref.at[rows_of(ysel[k] * 2 + 1 - c, mrows), :], mrc.at[k], c_peer,
            ms_.at[k], mr_.at[k],
        )

    def core(d, col, k):
        i = d * 4 + col * 2 + k
        xx = (1 - x, x)[col]
        at = mine(d, xx, ysel[k], 1 - c)
        go(moe_ref.at[at[0], at[1]], rc.at[i], c_peer, cs_.at[i], cr_.at[i])

    core(order[0], 0, 0)
    core(order[0], 0, 1)
    mixer_core(0)
    for d in order[1:]:
        core(d, 0, 0)
        core(d, 0, 1)
    for d in order:
        core(d, 1, 0)
        core(d, 1, 1)
    mixer_core(1)

    def pair(d, col, k):
        i = d * 4 + col * 2 + k
        xx = (1 - x, x)[col]
        at = mine(d, xx, ysel[k], c)
        got(rc.at[i], cr_.at[i])
        return moe_ref[at[0], at[1]].astype(f32) + rc[i].astype(f32)

    def x_send(d):
        for k in (0, 1):
            i = d * 2 + k
            s1[i] = pair(d, 0, k).astype(jnp.bfloat16)
            go(s1.at[i], rx.at[i], x_peer, xs_.at[i], xr_.at[i])

    x_send(order[0])
    got(mrc.at[0], mr_.at[0])
    ms[...] = (
        mix_ref[rows_of(ysel[0] * 2 + c, mrows), :].astype(f32) + mrc[0].astype(f32)
    ).astype(jnp.bfloat16)
    go(ms, mry, y_peer, ms_.at[2], mr_.at[2])
    for d in order[1:]:
        x_send(d)
    for d in order:
        for k in (0, 1):
            i = d * 2 + k
            part = pair(d, 1, k)
            got(rx.at[i], xr_.at[i])
            part = part + rx[i].astype(f32)
            if k == 0:
                s2[d] = part.astype(jnp.bfloat16)
                go(s2.at[d], ry.at[d], y_peer, ys_.at[d], yr_.at[d])
            else:
                keep[d] = part
    for d in order[:3]:
        got(ry.at[d], yr_.at[d])
        s3[d] = (keep[d] + ry[d].astype(f32)).astype(jnp.bfloat16)
        go(s3.at[d], rz.at[d], z_peer[d], zs_.at[d], zr_.at[d])
    got(mrc.at[1], mr_.at[1])
    got(mry, mr_.at[2])
    mix_out[...] = (
        mix_ref[rows_of(ysel[1] * 2 + c, mrows), :].astype(f32)
        + mrc[1].astype(f32)
        + mry[...].astype(f32)
    ).astype(jnp.bfloat16)
    got(ry.at[0], yr_.at[0])
    total = keep[0] + ry[0].astype(f32)
    for d in order[:3]:
        got(rz.at[d], zr_.at[d])
        total = total + rz[d].astype(f32)
    moe_out[...] = total.astype(jnp.bfloat16)
    for k in started:
        k.wait_send()


def reduce_both(moe, mix, n_ep):
    rows, width = moe.shape[0] // n_ep, moe.shape[1] // 4
    mrows, wide = mix.shape[0] // 4, mix.shape[1]
    dma = pltpu.SemaphoreType.DMA
    vm = pl.BlockSpec(memory_space=pltpu.VMEM)
    bf = jnp.bfloat16
    return pl.pallas_call(
        reduce_kernel,
        out_shape=(
            jax.ShapeDtypeStruct((rows, width), bf),
            jax.ShapeDtypeStruct((mrows, wide), bf),
        ),
        in_specs=[vm, vm],
        out_specs=(vm, vm),
        scratch_shapes=[
            pltpu.VMEM((16, rows, width), bf),
            pltpu.VMEM((8, rows, width), bf),
            pltpu.VMEM((8, rows, width), bf),
            pltpu.VMEM((4, rows, width), bf),
            pltpu.VMEM((4, rows, width), jnp.float32),
            pltpu.VMEM((4, rows, width), bf),
            pltpu.VMEM((4, rows, width), bf),
            pltpu.VMEM((4, rows, width), bf),
            pltpu.VMEM((2, mrows, wide), bf),
            pltpu.VMEM((mrows, wide), bf),
            pltpu.VMEM((mrows, wide), bf),
            dma((16,)), dma((16,)), dma((8,)), dma((8,)), dma((4,)), dma((4,)),
            dma((4,)), dma((4,)), dma((3,)), dma((3,)),
        ],
        compiler_params=pltpu.CompilerParams(
            collective_id=1, has_side_effects=True, vmem_limit_bytes=40 * 1024 * 1024
        ),
        name="reduce_both",
    )(moe, mix)


def local(
    tokens_first,
    attn_gain,
    w_query,
    key_matrix,
    value_matrix,
    head_sink_logit,
    w_output,
    tokens_second,
    ffn_gain,
    routes,
    route_weight,
    w_gate_exp,
    w_up_exp,
    w_down_exp,
    w_gate_shared,
    w_up_shared,
    w_down_shared,
):
    rows_first = tokens_first.shape[0]
    norm_input = rms_scale(tokens_first, attn_gain)
    offset = lax.axis_index("ep") * rows_first
    token_positions = (offset + jnp.arange(rows_first, dtype=jnp.int32)).astype(jnp.float32)
    head_count = w_query.shape[1] // HEAD_SIZE
    key_heads = key_matrix.shape[1] // HEAD_SIZE
    head_group = head_count // key_heads
    query_rows = apply_rotary(
        jnp.dot(norm_input, w_query, preferred_element_type=jnp.float32).reshape(
            rows_first, head_count, HEAD_SIZE
        ),
        token_positions,
    ).astype(jnp.bfloat16)
    keys_local = apply_rotary(
        jnp.dot(norm_input, key_matrix, preferred_element_type=jnp.float32).reshape(
            rows_first, key_heads, HEAD_SIZE
        ),
        token_positions,
    ).astype(jnp.bfloat16)
    values_local = (
        jnp.dot(norm_input, value_matrix, preferred_element_type=jnp.float32)
        .astype(jnp.bfloat16)
        .reshape(rows_first, key_heads, HEAD_SIZE)
    )
    kernels = lax.axis_size("ep") == 8 and lax.axis_size("tp") == 4
    if kernels:
        normed_second = rms_scale(tokens_second, ffn_gain)
        meta = jnp.concatenate([routes.astype(jnp.float32), route_weight], axis=1).T
        halo = jnp.concatenate(
            [
                keys_local[rows_first - BAND_LENGTH :].reshape(BAND_LENGTH, -1),
                values_local[rows_first - BAND_LENGTH :].reshape(BAND_LENGTH, -1),
            ],
            axis=1,
        )
        gathered, metas, before = gather(normed_second, meta, halo, lax.axis_size("ep"))
        split = key_heads * HEAD_SIZE
        keys_before = before[:, :split].reshape(BAND_LENGTH, key_heads, HEAD_SIZE)
        values_before = before[:, split:].reshape(BAND_LENGTH, key_heads, HEAD_SIZE)
    else:
        keys_before, values_before = from_behind(
            (keys_local[rows_first - BAND_LENGTH :], values_local[rows_first - BAND_LENGTH :]),
            "ep",
            1,
        )
    keys_all = jnp.concatenate([keys_before, keys_local], axis=0)
    values_all = jnp.concatenate([values_before, values_local], axis=0)
    layer_block = min(512, rows_first)
    sink_scores = head_sink_logit.reshape(key_heads, head_group)[:, :, None, None]

    def attend(index):
        leading_row = index * layer_block
        block_queries = query_rows.reshape(layer_block, key_heads, head_group, HEAD_SIZE)
        scores = jnp.einsum(
            "qhgd,khd->hgqk", block_queries, keys_all, preferred_element_type=jnp.float32
        ) * HEAD_SIZE ** (-0.5)
        query_pos = offset + leading_row + jnp.arange(layer_block, dtype=jnp.int32)
        key_pos = (
            offset
            + leading_row
            - BAND_LENGTH
            + jnp.arange(layer_block + BAND_LENGTH, dtype=jnp.int32)
        )
        offsets = query_pos[:, None] - key_pos[None, :]
        visible = (offsets >= 0) & (offsets < BAND_LENGTH) & (key_pos[None, :] >= 0)
        scores = jnp.where(visible[None, None], scores, -jnp.inf)
        peak = jnp.maximum(jnp.max(scores, axis=-1, keepdims=True), sink_scores)
        expo = jnp.exp(scores - peak)
        total = jnp.sum(expo, axis=-1, keepdims=True) + jnp.exp(sink_scores - peak)
        weights = (expo / total).astype(jnp.bfloat16)
        mixed = jnp.einsum(
            "hgqk,khd->qhgd", weights, values_all, preferred_element_type=jnp.float32
        )
        return mixed.astype(jnp.bfloat16).reshape(layer_block, head_count * HEAD_SIZE)

    attended = lax.map(attend, jnp.arange(rows_first // layer_block, dtype=jnp.int32)).reshape(
        rows_first, head_count * HEAD_SIZE
    )
    if kernels:
        capacity = max(2, 2 * tokens_second.shape[0] * routes.shape[1] // (w_gate_exp.shape[0] * 8))
        mixer_part = jnp.dot(attended, w_output, preferred_element_type=jnp.float32).astype(
            jnp.bfloat16
        )
        moe_part = experts_of(
            gathered, metas, w_gate_exp, w_up_exp, w_down_exp,
            w_gate_shared, w_up_shared, w_down_shared, capacity,
        )
        moe_out, mixer_out = reduce_both(moe_part, mixer_part, lax.axis_size("ep"))
        return (mixer_out, moe_out)
    mixer_out = lax.psum_scatter(
        jnp.dot(attended, w_output, preferred_element_type=jnp.float32).astype(jnp.bfloat16),
        "tp",
        scatter_dimension=0,
        tiled=True,
    )
    rows_second = tokens_second.shape[0]
    topk = routes.shape[1]
    exp_dev = w_gate_exp.shape[0]
    n_expdev = lax.axis_size("ep")
    experts = exp_dev * n_expdev
    capacity = max(2, 2 * rows_second * topk // experts)
    slot_count = experts * capacity
    normed_second = rms_scale(tokens_second, ffn_gain)
    flat = routes.reshape(-1)
    onehot = (flat[:, None] == jnp.arange(experts, dtype=jnp.int32)[None, :]).astype(jnp.int32)
    ranks = jnp.sum((jnp.cumsum(onehot, axis=0) - onehot) * onehot, axis=1)
    slots = flat * capacity + ranks
    match = (jnp.arange(slot_count, dtype=jnp.int32)[:, None] == slots[None, :]).reshape(
        slot_count, rows_second, topk
    )
    dispatch = jnp.sum(match.astype(jnp.float32), axis=2).astype(jnp.bfloat16)
    combine = jnp.sum(match.astype(jnp.float32) * route_weight[None, :, :], axis=2)
    width = normed_second.shape[1] // lax.axis_size("tp")
    feature_slice = lax.dynamic_slice_in_dim(normed_second, lax.axis_index("tp") * width, width, 1)
    outgoing = jnp.dot(dispatch, feature_slice, preferred_element_type=jnp.float32).astype(
        jnp.bfloat16
    )
    arrived = lax.all_to_all(outgoing, "ep", split_axis=0, concat_axis=0, tiled=True)
    piece = lax.all_gather(arrived, "tp", axis=1, tiled=True)
    cols = piece.shape[1]
    part = piece.reshape(n_expdev, exp_dev, capacity, cols)
    gate_pre = jnp.einsum("sjcd,jdf->sjcf", part, w_gate_exp, preferred_element_type=jnp.float32)
    up_pre = jnp.einsum("sjcd,jdf->sjcf", part, w_up_exp, preferred_element_type=jnp.float32)
    hidden = (jax.nn.silu(gate_pre) * up_pre).astype(jnp.bfloat16)
    shared_hidden = (
        jax.nn.silu(jnp.dot(normed_second, w_gate_shared, preferred_element_type=jnp.float32))
        * jnp.dot(normed_second, w_up_shared, preferred_element_type=jnp.float32)
    ).astype(jnp.bfloat16)
    routed_term = jnp.einsum(
        "sjcf,jfd->dsjc", hidden, w_down_exp, preferred_element_type=jnp.float32
    ).reshape(lax.axis_size("tp") * (MODEL_WIDTH // lax.axis_size("tp")), slot_count)
    shared_term = lax.dot_general(
        w_down_shared, shared_hidden, (((0,), (1,)), ((), ())), preferred_element_type=jnp.float32
    )
    summed = lax.psum_scatter(
        jnp.concatenate([routed_term, shared_term], axis=1).astype(jnp.bfloat16),
        "tp",
        scatter_dimension=0,
        tiled=True,
    ).astype(jnp.float32)
    routed_part = summed[:, :slot_count].astype(jnp.bfloat16)
    returned = lax.all_to_all(routed_part, "ep", split_axis=1, concat_axis=1, tiled=True)
    weighted = lax.dot_general(
        combine,
        returned.astype(jnp.float32),
        (((0,), (1,)), ((), ())),
        precision=lax.Precision.HIGHEST,
    )
    moe_out = (weighted + summed[:, slot_count:].T).astype(jnp.bfloat16)
    return (mixer_out, moe_out)


def solution(mesh):
    in_specs = (
        P("ep", None),
        P(),
        P(None, "tp"),
        P(None, "tp"),
        P(None, "tp"),
        P("tp"),
        P("tp", None),
        P("ep", None),
        P(),
        P("ep", None),
        P("ep", None),
        P("ep", None, "tp"),
        P("ep", None, "tp"),
        P("ep", "tp", None),
        P(None, "tp"),
        P(None, "tp"),
        P("tp", None),
    )
    out_specs = (P(("ep", "tp"), None), P("ep", "tp"))
    return jax.shard_map(local, mesh=mesh, in_specs=in_specs, out_specs=out_specs, check_vma=False)
```

```python
import functools
import jax
import jax.numpy as jnp
from jax import lax
from jax.experimental import pallas as pl
from jax.experimental.pallas import tpu as pltpu
from jax.sharding import PartitionSpec as P

MODEL_WIDTH = 2048
HEAD_SIZE = 64
BAND_LENGTH = 128


rope_base = 10000.0
norm_eps = 1e-06


def from_behind(value, axis, by):
    devices = lax.axis_size(axis)
    pairs = [(i, i + by) for i in range(devices) if 0 <= i + by < devices]
    return lax.ppermute(value, axis, pairs)


def rms_scale(inputs, gain):
    wide = inputs.astype(jnp.float32)
    scaled = wide * lax.rsqrt(jnp.mean(wide * wide, axis=-1, keepdims=True) + norm_eps)
    return (scaled * gain).astype(jnp.bfloat16)


def apply_rotary(heads, token_positions):
    freqs = rope_base ** (-jnp.arange(0, HEAD_SIZE, 2, dtype=jnp.float32) / HEAD_SIZE)
    angles = token_positions[:, None] * freqs[None, :]
    cosine = jnp.cos(angles)[:, None, :]
    sine = jnp.sin(angles)[:, None, :]
    first_half, second_half = jnp.split(heads, 2, axis=-1)
    return jnp.concatenate(
        [first_half * cosine - second_half * sine, second_half * cosine + first_half * sine],
        axis=-1,
    )


MESH = pl.DeviceIdType.MESH


def whereabouts():
    me, t = lax.axis_index("ep"), lax.axis_index("tp")
    z, x, y, c = me // 2, me % 2, t // 2, t % 2
    zs = (z, z + 1 - 2 * (z % 2), (z + 2) % 4, 3 - z)
    return me, x, y, c, zs


def cols(yy, cc, width):
    return pl.ds(pl.multiple_of((yy * 2 + cc) * width, 128), width)


def rows_of(index, count):
    return pl.ds(pl.multiple_of(index * count, 16), count)


def gather_kernel(
    n_ep, x_ref, meta_ref, halo_ref, out_ref, meta_out, halo_out,
    zs_, zr_, xs_, xr_, ys_, yr_, cs_, cr_, ms_, mr_, hs_, hr_,
):
    me, x, y, c, zs = whereabouts()
    rows, width = x_ref.shape[0], x_ref.shape[1] // 4
    z_peer = [{"ep": zd * 2 + x, "tp": y * 2 + c} for zd in zs]
    x_peer = {"ep": zs[0] * 2 + 1 - x, "tp": y * 2 + c}
    y_peer = {"ep": me, "tp": (1 - y) * 2 + c}
    c_peer = {"ep": me, "tp": y * 2 + 1 - c}
    barrier = pltpu.get_barrier_semaphore()
    for e in range(1, n_ep):
        pl.semaphore_signal(
            barrier, inc=1, device_id={"ep": (me + e) % n_ep, "tp": y * 2 + c}, device_id_type=MESH
        )
    for peer in (y_peer, c_peer):
        pl.semaphore_signal(barrier, inc=1, device_id=peer, device_id_type=MESH)
    pl.semaphore_wait(barrier, n_ep + 1)

    started = []

    def make(blk, yy, peer, send, recv, own=False):
        at = out_ref.at[rows_of(blk, rows), cols(yy, c, width)]
        return pltpu.make_async_remote_copy(
            src_ref=x_ref.at[:, cols(yy, c, width)] if own else at,
            dst_ref=at, send_sem=send, recv_sem=recv, device_id=peer, device_id_type=MESH,
        )

    def go(*a, **k):
        copy = make(*a, **k)
        copy.start()
        started.append(copy)

    for d in (1, 2, 3):
        go(me, y, z_peer[d], zs_.at[d], zr_.at[d], own=True)
        if d == 1:
            go(me, y, x_peer, xs_.at[0], xr_.at[0], own=True)
    go(me, 1 - y, z_peer[1], zs_.at[0], zr_.at[0], own=True)
    go(me, 1 - y, x_peer, xs_.at[4], xr_.at[4], own=True)

    def meta_copy(e, to):
        return pltpu.make_async_remote_copy(
            src_ref=meta_ref, dst_ref=meta_out.at[to], send_sem=ms_.at[e], recv_sem=mr_.at[e],
            device_id={"ep": (me + e) % n_ep, "tp": y * 2 + c}, device_id_type=MESH,
        )

    for e in range(1, n_ep):
        meta_copy(e, me).start()
    halo = pltpu.make_async_remote_copy(
        src_ref=halo_ref, dst_ref=halo_out, send_sem=hs_, recv_sem=hr_,
        device_id={"ep": (me + 1) % n_ep, "tp": y * 2 + c}, device_id_type=MESH,
    )

    @pl.when(me < n_ep - 1)
    def _():
        halo.start()

    @pl.when(me == 0)
    def _():
        halo_out[...] = jnp.zeros_like(halo_out)

    out_ref[rows_of(me, rows), :] = x_ref[...]
    meta_out[me] = meta_ref[...]

    c_list = []

    def arrived(blk, yy, sem, peer):
        make(blk, yy, peer, sem, sem).wait_recv()

    def to_core(blk, yy):
        i = len(c_list)
        c_list.append((blk, yy))
        go(blk, yy, c_peer, cs_.at[i], cr_.at[i])

    y_list = []

    def to_y(blk):
        i = len(y_list)
        y_list.append(blk)
        go(blk, y, y_peer, ys_.at[i], yr_.at[i])

    def blk(d, xx):
        return zs[d] * 2 + xx

    for d in (1, 2, 3):
        arrived(blk(d, x), y, zr_.at[d], c_peer)
        go(blk(d, x), y, x_peer, xs_.at[d], xr_.at[d])
        if d != 1:
            to_y(blk(d, x))
        to_core(blk(d, x), y)
        if d == 1:
            arrived(blk(0, 1 - x), y, xr_.at[0], c_peer)
            to_core(blk(0, 1 - x), y)
        if d == 2:
            arrived(blk(0, 1 - x), 1 - y, xr_.at[4], c_peer)
            to_core(blk(0, 1 - x), 1 - y)
    arrived(blk(1, x), 1 - y, zr_.at[0], c_peer)
    to_core(blk(1, x), 1 - y)
    for d in (1, 2, 3):
        arrived(blk(d, 1 - x), y, xr_.at[d], c_peer)
        to_y(blk(d, 1 - x))
        to_core(blk(d, 1 - x), y)
    for i, b in enumerate(list(y_list)):
        arrived(b, 1 - y, yr_.at[i], c_peer)
        to_core(b, 1 - y)
    for i, (b, yy) in enumerate(c_list):
        at = out_ref.at[rows_of(b, rows), cols(yy, 1 - c, width)]
        pltpu.make_async_remote_copy(
            src_ref=at, dst_ref=at, send_sem=cs_.at[i], recv_sem=cr_.at[i],
            device_id=c_peer, device_id_type=MESH,
        ).wait_recv()
    for e in range(1, n_ep):
        meta_copy(e, (me + n_ep - e) % n_ep).wait_recv()

    @pl.when(me > 0)
    def _():
        halo.wait_recv()

    @pl.when(me < n_ep - 1)
    def _():
        halo.wait_send()

    for copy in started:
        copy.wait_send()
    for e in range(1, n_ep):
        meta_copy(e, me).wait_send()


def gather(x, meta, halo, n_ep):
    rows, wide = x.shape
    dma = pltpu.SemaphoreType.DMA
    vm = pl.BlockSpec(memory_space=pltpu.VMEM)
    return pl.pallas_call(
        functools.partial(gather_kernel, n_ep),
        out_shape=(
            jax.ShapeDtypeStruct((n_ep * rows, wide), x.dtype),
            jax.ShapeDtypeStruct((n_ep,) + meta.shape, meta.dtype),
            jax.ShapeDtypeStruct(halo.shape, halo.dtype),
        ),
        in_specs=[vm] * 3,
        out_specs=(vm, vm, vm),
        scratch_shapes=[
            dma((4,)), dma((4,)), dma((5,)), dma((5,)), dma((5,)), dma((5,)),
            dma((14,)), dma((14,)), dma((n_ep,)), dma((n_ep,)), dma, dma,
        ],
        compiler_params=pltpu.CompilerParams(
            collective_id=0, has_side_effects=True, vmem_limit_bytes=40 * 1024 * 1024
        ),
        name="gather_rows",
    )(x, meta, halo)


def ffn_kernel(
    cap, x_ref, meta_ref, wg_ref, wu_ref, wd_ref, sg_ref, su_ref, sd_ref, out_ref, xs, ys
):
    w_count = ys.shape[1] // cap
    j = pl.program_id(0)
    exp_dev = pl.num_programs(0)
    me = lax.axis_index("ep")
    n_ep, _, rows = meta_ref.shape
    topk = meta_ref.shape[1] // 2
    f32 = jnp.float32
    before = (
        lax.broadcasted_iota(jnp.int32, (rows, rows), 0)
        < lax.broadcasted_iota(jnp.int32, (rows, rows), 1)
    ).astype(f32).astype(jnp.bfloat16)

    def placed(s, jj, weighted):
        e = (me * exp_dev + jj).astype(f32)
        named = meta_ref[s, 0:topk, :] == e
        hit = jnp.sum(named.astype(f32), axis=0, keepdims=True)
        rank = jnp.dot(
            jnp.broadcast_to(hit, (16, rows)).astype(jnp.bfloat16), before,
            preferred_element_type=f32,
        )[0:1]
        slot = lax.broadcasted_iota(jnp.int32, (cap, rows), 0).astype(f32)
        value = hit
        if weighted:
            value = jnp.sum(
                jnp.where(named, meta_ref[s, topk : 2 * topk, :], 0.0), axis=0, keepdims=True
            )
        return jnp.where((slot == rank) & (hit > 0.0), value, 0.0)

    for s in range(n_ep):
        xs[pl.ds(s * cap, cap), :] = jnp.dot(
            placed(s, j, False).astype(jnp.bfloat16), x_ref[pl.ds(s * rows, rows), :],
            preferred_element_type=f32,
        ).astype(jnp.bfloat16)
    rows_in = xs[...]
    gate = jnp.dot(rows_in, wg_ref[0], preferred_element_type=f32)
    up = jnp.dot(rows_in, wu_ref[0], preferred_element_type=f32)
    hidden = (gate / (1.0 + jnp.exp(-gate)) * up).astype(jnp.bfloat16)
    res = jnp.dot(hidden, wd_ref[0], preferred_element_type=f32).astype(jnp.bfloat16)
    for s in range(n_ep):
        ys[s, pl.ds(pl.multiple_of(j * cap, cap), cap), :] = res[s * cap : (s + 1) * cap]

    @pl.when(j == exp_dev - 1)
    def _():
        for s in range(n_ep):
            mix = jnp.concatenate([placed(s, jj, True) for jj in range(w_count)], axis=0)
            out_ref[pl.ds(s * rows, rows), :] = jnp.dot(
                mix.T.astype(jnp.bfloat16), ys[s], preferred_element_type=f32
            ).astype(jnp.bfloat16)
        mine = rows_of(me, rows)
        own = x_ref[mine, :]
        sg = jnp.dot(own, sg_ref[...], preferred_element_type=f32)
        su = jnp.dot(own, su_ref[...], preferred_element_type=f32)
        sh = (sg / (1.0 + jnp.exp(-sg)) * su).astype(jnp.bfloat16)
        out_ref[mine, :] = (
            out_ref[mine, :].astype(f32) + jnp.dot(sh, sd_ref[...], preferred_element_type=f32)
        ).astype(jnp.bfloat16)


def experts_of(x, meta, wg, wu, wd, sg, su, sd, cap):
    n_ep, _, rows = meta.shape
    exp_dev, wide, hid = wg.shape
    vm = pl.BlockSpec(memory_space=pltpu.VMEM)
    return pl.pallas_call(
        functools.partial(ffn_kernel, cap),
        grid=(exp_dev,),
        out_shape=jax.ShapeDtypeStruct(x.shape, jnp.bfloat16),
        in_specs=[
            vm, vm,
            pl.BlockSpec((1, wide, hid), lambda j: (j, 0, 0)),
            pl.BlockSpec((1, wide, hid), lambda j: (j, 0, 0)),
            pl.BlockSpec((1, hid, wide), lambda j: (j, 0, 0)),
            vm, vm, vm,
        ],
        out_specs=vm,
        scratch_shapes=[
            pltpu.VMEM((n_ep * cap, wide), jnp.bfloat16),
            pltpu.VMEM((n_ep, exp_dev * cap, wide), jnp.bfloat16),
        ],
        compiler_params=pltpu.CompilerParams(
            dimension_semantics=("arbitrary",), vmem_limit_bytes=58 * 1024 * 1024
        ),
        name="experts",
    )(x, meta, wg, wu, wd, sg, su, sd)


def reduce_kernel(
    moe_ref, mix_ref, moe_out, mix_out, rc, s1, rx, s2, keep, ry, s3, rz, mrc, ms, mry,
    cs_, cr_, xs_, xr_, ys_, yr_, zs_, zr_, ms_, mr_,
):
    me, x, y, c, zs = whereabouts()
    rows, width = moe_out.shape
    mrows = mix_out.shape[0]
    f32 = jnp.float32
    x_peer = {"ep": zs[0] * 2 + 1 - x, "tp": y * 2 + c}
    y_peer = {"ep": me, "tp": (1 - y) * 2 + c}
    c_peer = {"ep": me, "tp": y * 2 + 1 - c}
    z_peer = [{"ep": zd * 2 + x, "tp": y * 2 + c} for zd in zs]
    barrier = pltpu.get_barrier_semaphore()
    for peer in [x_peer, y_peer, c_peer] + z_peer[1:]:
        pl.semaphore_signal(barrier, inc=1, device_id=peer, device_id_type=MESH)
    pl.semaphore_wait(barrier, 6)
    started = []

    def copy(src, dst, peer, send, recv):
        return pltpu.make_async_remote_copy(
            src_ref=src, dst_ref=dst, send_sem=send, recv_sem=recv,
            device_id=peer, device_id_type=MESH,
        )

    def go(*a):
        k = copy(*a)
        k.start()
        started.append(k)

    def got(dst, recv):
        copy(dst, dst, c_peer, recv, recv).wait_recv()

    ysel = (1 - y, y)
    order = (2, 3, 1, 0)

    def mine(d, xx, yy, cc):
        return (rows_of(zs[d] * 2 + xx, rows), cols(yy, cc, width))

    def mixer_core(k):
        go(
            mix_ref.at[rows_of(ysel[k] * 2 + 1 - c, mrows), :], mrc.at[k], c_peer,
            ms_.at[k], mr_.at[k],
        )

    def core(d, col, k):
        i = d * 4 + col * 2 + k
        xx = (1 - x, x)[col]
        at = mine(d, xx, ysel[k], 1 - c)
        go(moe_ref.at[at[0], at[1]], rc.at[i], c_peer, cs_.at[i], cr_.at[i])

    core(order[0], 0, 0)
    core(order[0], 0, 1)
    mixer_core(0)
    for d in order[1:]:
        core(d, 0, 0)
        core(d, 0, 1)
    for d in order:
        core(d, 1, 0)
        core(d, 1, 1)
    mixer_core(1)

    def pair(d, col, k):
        i = d * 4 + col * 2 + k
        xx = (1 - x, x)[col]
        at = mine(d, xx, ysel[k], c)
        got(rc.at[i], cr_.at[i])
        return moe_ref[at[0], at[1]].astype(f32) + rc[i].astype(f32)

    def x_send(d):
        for k in (0, 1):
            i = d * 2 + k
            s1[i] = pair(d, 0, k).astype(jnp.bfloat16)
            go(s1.at[i], rx.at[i], x_peer, xs_.at[i], xr_.at[i])

    x_send(order[0])
    got(mrc.at[0], mr_.at[0])
    ms[...] = (
        mix_ref[rows_of(ysel[0] * 2 + c, mrows), :].astype(f32) + mrc[0].astype(f32)
    ).astype(jnp.bfloat16)
    go(ms, mry, y_peer, ms_.at[2], mr_.at[2])
    for d in order[1:]:
        x_send(d)
    for d in order:
        for k in (0, 1):
            i = d * 2 + k
            part = pair(d, 1, k)
            got(rx.at[i], xr_.at[i])
            part = part + rx[i].astype(f32)
            if k == 0:
                s2[d] = part.astype(jnp.bfloat16)
                go(s2.at[d], ry.at[d], y_peer, ys_.at[d], yr_.at[d])
            else:
                keep[d] = part
    for d in order[:3]:
        got(ry.at[d], yr_.at[d])
        s3[d] = (keep[d] + ry[d].astype(f32)).astype(jnp.bfloat16)
        go(s3.at[d], rz.at[d], z_peer[d], zs_.at[d], zr_.at[d])
    got(mrc.at[1], mr_.at[1])
    got(mry, mr_.at[2])
    mix_out[...] = (
        mix_ref[rows_of(ysel[1] * 2 + c, mrows), :].astype(f32)
        + mrc[1].astype(f32)
        + mry[...].astype(f32)
    ).astype(jnp.bfloat16)
    got(ry.at[0], yr_.at[0])
    total = keep[0] + ry[0].astype(f32)
    for d in order[:3]:
        got(rz.at[d], zr_.at[d])
        total = total + rz[d].astype(f32)
    moe_out[...] = total.astype(jnp.bfloat16)
    for k in started:
        k.wait_send()


def reduce_both(moe, mix, n_ep):
    rows, width = moe.shape[0] // n_ep, moe.shape[1] // 4
    mrows, wide = mix.shape[0] // 4, mix.shape[1]
    dma = pltpu.SemaphoreType.DMA
    vm = pl.BlockSpec(memory_space=pltpu.VMEM)
    bf = jnp.bfloat16
    return pl.pallas_call(
        reduce_kernel,
        out_shape=(
            jax.ShapeDtypeStruct((rows, width), bf),
            jax.ShapeDtypeStruct((mrows, wide), bf),
        ),
        in_specs=[vm, vm],
        out_specs=(vm, vm),
        scratch_shapes=[
            pltpu.VMEM((16, rows, width), bf),
            pltpu.VMEM((8, rows, width), bf),
            pltpu.VMEM((8, rows, width), bf),
            pltpu.VMEM((4, rows, width), bf),
            pltpu.VMEM((4, rows, width), jnp.float32),
            pltpu.VMEM((4, rows, width), bf),
            pltpu.VMEM((4, rows, width), bf),
            pltpu.VMEM((4, rows, width), bf),
            pltpu.VMEM((2, mrows, wide), bf),
            pltpu.VMEM((mrows, wide), bf),
            pltpu.VMEM((mrows, wide), bf),
            dma((16,)), dma((16,)), dma((8,)), dma((8,)), dma((4,)), dma((4,)),
            dma((4,)), dma((4,)), dma((3,)), dma((3,)),
        ],
        compiler_params=pltpu.CompilerParams(
            collective_id=1, has_side_effects=True, vmem_limit_bytes=40 * 1024 * 1024
        ),
        name="reduce_both",
    )(moe, mix)


def local(
    tokens_first,
    attn_gain,
    w_query,
    key_matrix,
    value_matrix,
    head_sink_logit,
    w_output,
    tokens_second,
    ffn_gain,
    routes,
    route_weight,
    w_gate_exp,
    w_up_exp,
    w_down_exp,
    w_gate_shared,
    w_up_shared,
    w_down_shared,
):
    rows_first = tokens_first.shape[0]
    norm_input = rms_scale(tokens_first, attn_gain)
    offset = lax.axis_index("ep") * rows_first
    token_positions = (offset + jnp.arange(rows_first, dtype=jnp.int32)).astype(jnp.float32)
    head_count = w_query.shape[1] // HEAD_SIZE
    key_heads = key_matrix.shape[1] // HEAD_SIZE
    head_group = head_count // key_heads
    query_rows = apply_rotary(
        jnp.dot(norm_input, w_query, preferred_element_type=jnp.float32).reshape(
            rows_first, head_count, HEAD_SIZE
        ),
        token_positions,
    ).astype(jnp.bfloat16)
    keys_local = apply_rotary(
        jnp.dot(norm_input, key_matrix, preferred_element_type=jnp.float32).reshape(
            rows_first, key_heads, HEAD_SIZE
        ),
        token_positions,
    ).astype(jnp.bfloat16)
    values_local = (
        jnp.dot(norm_input, value_matrix, preferred_element_type=jnp.float32)
        .astype(jnp.bfloat16)
        .reshape(rows_first, key_heads, HEAD_SIZE)
    )
    kernels = lax.axis_size("ep") == 8 and lax.axis_size("tp") == 4
    if kernels:
        normed_second = rms_scale(tokens_second, ffn_gain)
        meta = jnp.concatenate([routes.astype(jnp.float32), route_weight], axis=1).T
        halo = jnp.concatenate(
            [
                keys_local[rows_first - BAND_LENGTH :].reshape(BAND_LENGTH, -1),
                values_local[rows_first - BAND_LENGTH :].reshape(BAND_LENGTH, -1),
            ],
            axis=1,
        )
        gathered, metas, before = gather(normed_second, meta, halo, lax.axis_size("ep"))
        split = key_heads * HEAD_SIZE
        keys_before = before[:, :split].reshape(BAND_LENGTH, key_heads, HEAD_SIZE)
        values_before = before[:, split:].reshape(BAND_LENGTH, key_heads, HEAD_SIZE)
    else:
        keys_before, values_before = from_behind(
            (keys_local[rows_first - BAND_LENGTH :], values_local[rows_first - BAND_LENGTH :]),
            "ep",
            1,
        )
    keys_all = jnp.concatenate([keys_before, keys_local], axis=0)
    values_all = jnp.concatenate([values_before, values_local], axis=0)
    band = BAND_LENGTH
    bands = rows_first // band

    def windows(padded):
        return jnp.concatenate(
            [
                padded[:rows_first].reshape(bands, band, key_heads, HEAD_SIZE),
                padded[band:].reshape(bands, band, key_heads, HEAD_SIZE),
            ],
            axis=1,
        )

    sink_scores = head_sink_logit.reshape(key_heads, head_group)[None, :, :, None, None]
    scores = jnp.einsum(
        "bqhgd,bkhd->bhgqk",
        query_rows.reshape(bands, band, key_heads, head_group, HEAD_SIZE),
        windows(keys_all),
        preferred_element_type=jnp.float32,
    ) * HEAD_SIZE ** (-0.5)
    offsets = (
        band
        + jnp.arange(band, dtype=jnp.int32)[:, None]
        - jnp.arange(2 * band, dtype=jnp.int32)[None, :]
    )
    key_pos = (
        offset
        + (jnp.arange(bands, dtype=jnp.int32)[:, None] - 1) * band
        + jnp.arange(2 * band, dtype=jnp.int32)[None, :]
    )
    visible = ((offsets >= 0) & (offsets < band))[None] & (key_pos >= 0)[:, None, :]
    scores = jnp.where(visible[:, None, None], scores, -jnp.inf)
    peak = jnp.maximum(jnp.max(scores, axis=-1, keepdims=True), sink_scores)
    expo = jnp.exp(scores - peak)
    total = jnp.sum(expo, axis=-1, keepdims=True) + jnp.exp(sink_scores - peak)
    weights = (expo / total).astype(jnp.bfloat16)
    attended = (
        jnp.einsum(
            "bhgqk,bkhd->bqhgd", weights, windows(values_all), preferred_element_type=jnp.float32
        )
        .astype(jnp.bfloat16)
        .reshape(rows_first, head_count * HEAD_SIZE)
    )
    if kernels:
        capacity = max(2, 2 * tokens_second.shape[0] * routes.shape[1] // (w_gate_exp.shape[0] * 8))
        mixer_part = jnp.dot(attended, w_output, preferred_element_type=jnp.float32).astype(
            jnp.bfloat16
        )
        moe_part = experts_of(
            gathered, metas, w_gate_exp, w_up_exp, w_down_exp,
            w_gate_shared, w_up_shared, w_down_shared, capacity,
        )
        moe_out, mixer_out = reduce_both(moe_part, mixer_part, lax.axis_size("ep"))
        return (mixer_out, moe_out)
    mixer_out = lax.psum_scatter(
        jnp.dot(attended, w_output, preferred_element_type=jnp.float32).astype(jnp.bfloat16),
        "tp",
        scatter_dimension=0,
        tiled=True,
    )
    rows_second = tokens_second.shape[0]
    topk = routes.shape[1]
    exp_dev = w_gate_exp.shape[0]
    n_expdev = lax.axis_size("ep")
    experts = exp_dev * n_expdev
    capacity = max(2, 2 * rows_second * topk // experts)
    slot_count = experts * capacity
    normed_second = rms_scale(tokens_second, ffn_gain)
    flat = routes.reshape(-1)
    onehot = (flat[:, None] == jnp.arange(experts, dtype=jnp.int32)[None, :]).astype(jnp.int32)
    ranks = jnp.sum((jnp.cumsum(onehot, axis=0) - onehot) * onehot, axis=1)
    slots = flat * capacity + ranks
    match = (jnp.arange(slot_count, dtype=jnp.int32)[:, None] == slots[None, :]).reshape(
        slot_count, rows_second, topk
    )
    dispatch = jnp.sum(match.astype(jnp.float32), axis=2).astype(jnp.bfloat16)
    combine = jnp.sum(match.astype(jnp.float32) * route_weight[None, :, :], axis=2)
    width = normed_second.shape[1] // lax.axis_size("tp")
    feature_slice = lax.dynamic_slice_in_dim(normed_second, lax.axis_index("tp") * width, width, 1)
    outgoing = jnp.dot(dispatch, feature_slice, preferred_element_type=jnp.float32).astype(
        jnp.bfloat16
    )
    arrived = lax.all_to_all(outgoing, "ep", split_axis=0, concat_axis=0, tiled=True)
    piece = lax.all_gather(arrived, "tp", axis=1, tiled=True)
    cols = piece.shape[1]
    part = piece.reshape(n_expdev, exp_dev, capacity, cols)
    gate_pre = jnp.einsum("sjcd,jdf->sjcf", part, w_gate_exp, preferred_element_type=jnp.float32)
    up_pre = jnp.einsum("sjcd,jdf->sjcf", part, w_up_exp, preferred_element_type=jnp.float32)
    hidden = (jax.nn.silu(gate_pre) * up_pre).astype(jnp.bfloat16)
    shared_hidden = (
        jax.nn.silu(jnp.dot(normed_second, w_gate_shared, preferred_element_type=jnp.float32))
        * jnp.dot(normed_second, w_up_shared, preferred_element_type=jnp.float32)
    ).astype(jnp.bfloat16)
    routed_term = jnp.einsum(
        "sjcf,jfd->dsjc", hidden, w_down_exp, preferred_element_type=jnp.float32
    ).reshape(lax.axis_size("tp") * (MODEL_WIDTH // lax.axis_size("tp")), slot_count)
    shared_term = lax.dot_general(
        w_down_shared, shared_hidden, (((0,), (1,)), ((), ())), preferred_element_type=jnp.float32
    )
    summed = lax.psum_scatter(
        jnp.concatenate([routed_term, shared_term], axis=1).astype(jnp.bfloat16),
        "tp",
        scatter_dimension=0,
        tiled=True,
    ).astype(jnp.float32)
    routed_part = summed[:, :slot_count].astype(jnp.bfloat16)
    returned = lax.all_to_all(routed_part, "ep", split_axis=1, concat_axis=1, tiled=True)
    weighted = lax.dot_general(
        combine,
        returned.astype(jnp.float32),
        (((0,), (1,)), ((), ())),
        precision=lax.Precision.HIGHEST,
    )
    moe_out = (weighted + summed[:, slot_count:].T).astype(jnp.bfloat16)
    return (mixer_out, moe_out)


def solution(mesh):
    in_specs = (
        P("ep", None),
        P(),
        P(None, "tp"),
        P(None, "tp"),
        P(None, "tp"),
        P("tp"),
        P("tp", None),
        P("ep", None),
        P(),
        P("ep", None),
        P("ep", None),
        P("ep", None, "tp"),
        P("ep", None, "tp"),
        P("ep", "tp", None),
        P(None, "tp"),
        P(None, "tp"),
        P("tp", None),
    )
    out_specs = (P(("ep", "tp"), None), P("ep", "tp"))
    return jax.shard_map(local, mesh=mesh, in_specs=in_specs, out_specs=out_specs, check_vma=False)
```
